512 devices in a mesh: sp: 64 (over z, y), tp: 8 (over x, core).
Axes of the slice: x: 4, y: 4, z: 16, core: 2. Of those that a mesh axis runs over, the one named last changes fastest.
Arguments:
- queries: bfloat16 [8192, 1024], P('sp', 'tp'), may hold values from -6 to 6
- attn_out: bfloat16 [8192, 1024], P('sp', 'tp'), may hold values from -6 to 6
- out_grad: bfloat16 [8192, 1024], P('sp', 'tp'), may hold values from -384 to 384
- row_lse: float32 [8192, 8], P('sp', 'tp'), may hold values from 9.5 to 12.5
- source: bfloat16 [32768, 4096], P('sp', 'tp'), may hold values from -6 to 6
- saved_keys: bfloat16 [32768, 256], P('sp'), may hold values from -6 to 6
- saved_values: bfloat16 [32768, 256], P('sp'), may hold values from -6 to 6
- key_weight: bfloat16 [4096, 256], P('tp'), may hold values from -0.09375 to 0.09375
- value_weight: bfloat16 [4096, 256], P('tp'), may hold values from -0.09375 to 0.09375
Outputs:
- query_grad: float32 [8192, 1024], P('sp', 'tp')
- source_grad: float32 [32768, 4096], P('sp', 'tp')
- key_grad: float32 [256, 4096], P('sp', 'tp')
The draws below stay inside these ranges and needn't reach their ends.
All inputs are finite; a program needn't handle non-finite values.
Results may differ from the reference program's by a relative error of at most 0.012.
Values may be sent and summed in bfloat16 or wider, within the bound.
A program may use at most 64 MiB of HBM per device.

```python
import math
import jax
import jax.numpy as jnp
from jax import lax

D = 4096
HEADS = 8
KV_HEADS = 2
HEAD_DIM = 128
TARGET_ROWS = 8192
SOURCE_ROWS = 32768


def levels(rng, extent, cuts, smallest, largest):
    def one(position, parts):
        heights = jax.random.uniform(jax.random.fold_in(jax.random.fold_in(rng, 6), position), (parts,), jnp.float32, smallest / len(cuts), largest / len(cuts))
        return jnp.repeat(jnp.exp(heights), extent[position] // parts).reshape((-1,) + (1,) * (len(extent) - position - 1))

    gain = one(*cuts[0])
    for cut in cuts[1:]:
        gain = gain * one(*cut)
    return gain


def normal_values(rng, dims, deviation, reach, pieces=(), dtype=jnp.bfloat16):
    array = deviation * jax.random.normal(rng, dims, jnp.float32)
    if pieces:
        array = array * levels(rng, dims, pieces, -0.22, 0.18)
    return jnp.clip(array, -reach, reach).astype(dtype)


def setup_inputs(seed: int = 0) -> dict:
    arg_keys = jax.random.split(jax.random.key(seed), 10)
    return {
        "queries": normal_values(arg_keys[0], (TARGET_ROWS, HEADS * HEAD_DIM), 1.0, 6.0, ((0, 64), (1, 8))),
        "attn_out": normal_values(arg_keys[1], (TARGET_ROWS, HEADS * HEAD_DIM), 1.0, 6.0, ((0, 64), (1, 8))),
        "out_grad": normal_values(arg_keys[2], (TARGET_ROWS, HEADS * HEAD_DIM), 64.0, 384.0, ((0, 64), (1, 8))),
        "row_lse": jnp.clip(9.5 + 3.0 * jax.random.uniform(arg_keys[3], (TARGET_ROWS, HEADS), jnp.float32) ** levels(arg_keys[3], (TARGET_ROWS, HEADS), ((0, 64), (1, 8)), -0.2, 0.2), 9.5, 12.5),
        "source": normal_values(arg_keys[4], (SOURCE_ROWS, D), 1.0, 6.0, ((0, 64), (1, 8))),
        "saved_keys": normal_values(arg_keys[5], (SOURCE_ROWS, KV_HEADS * HEAD_DIM), 1.0, 6.0, ((0, 64),)),
        "saved_values": normal_values(arg_keys[6], (SOURCE_ROWS, KV_HEADS * HEAD_DIM), 1.0, 6.0, ((0, 64),)),
        "key_weight": normal_values(arg_keys[7], (D, KV_HEADS * HEAD_DIM), D ** -0.5, 0.09375, ((0, 8),)),
        "value_weight": normal_values(arg_keys[8], (D, KV_HEADS * HEAD_DIM), D ** -0.5, 0.09375, ((0, 8),)),
    }


def reference(queries, attn_out, out_grad, row_lse, source, saved_keys, saved_values, key_weight, value_weight):
    per_key = HEADS // KV_HEADS
    score_scale = 1.0 / math.sqrt(HEAD_DIM)
    tgt_len = queries.shape[0]
    src_len = source.shape[0]
    span = math.gcd(tgt_len, 1024)
    count = tgt_len // span
    row_delta = lax.optimization_barrier(jnp.sum((out_grad.astype(jnp.float32) * attn_out.astype(jnp.float32)).reshape(-1, HEADS, HEAD_DIM), axis=2))
    key_acc = jnp.zeros((src_len, KV_HEADS * HEAD_DIM), jnp.float32)
    value_acc = jnp.zeros((src_len, KV_HEADS * HEAD_DIM), jnp.float32)
    head_parts = []
    for head_index in range(HEADS):
        kv_lo = head_index // per_key * HEAD_DIM
        col_lo = head_index * HEAD_DIM
        key_head = saved_keys[:, kv_lo:kv_lo + HEAD_DIM]
        value_head = saved_values[:, kv_lo:kv_lo + HEAD_DIM]
        query_blocks = queries[:, col_lo:col_lo + HEAD_DIM].reshape(count, span, HEAD_DIM)
        grad_blocks = out_grad[:, col_lo:col_lo + HEAD_DIM].reshape(count, span, HEAD_DIM)
        lse_blocks = row_lse[:, head_index:head_index + 1].reshape(count, span, 1)
        delta_blocks = row_delta[:, head_index:head_index + 1].reshape(count, span, 1)

        def step(carry, items):
            key_part, value_part = carry
            query_head, grad_head, lse_col, delta_col = items
            scores = jnp.dot(query_head, key_head.T, preferred_element_type=jnp.float32) * score_scale
            attn_probs = jnp.exp(scores - lse_col)
            dprobs = jnp.dot(grad_head, value_head.T, preferred_element_type=jnp.float32)
            dscores = (attn_probs * (dprobs - delta_col) * score_scale).astype(jnp.bfloat16)
            key_part = key_part + jnp.dot(dscores.T, query_head, preferred_element_type=jnp.float32)
            value_part = value_part + jnp.dot(attn_probs.astype(jnp.bfloat16).T, grad_head, preferred_element_type=jnp.float32)
            return ((key_part, value_part), jnp.dot(dscores, key_head, preferred_element_type=jnp.float32))
        empty = jnp.zeros((src_len, HEAD_DIM), jnp.float32)
        (key_part, value_part), query_blocks_out = lax.scan(step, (empty, empty), (query_blocks, grad_blocks, lse_blocks, delta_blocks))
        head_parts.append(query_blocks_out.reshape(tgt_len, HEAD_DIM))
        key_acc = key_acc.at[:, kv_lo:kv_lo + HEAD_DIM].add(key_part)
        value_acc = value_acc.at[:, kv_lo:kv_lo + HEAD_DIM].add(value_part)
    query_grad = jnp.concatenate(head_parts, axis=1)
    key_half = key_acc.astype(jnp.bfloat16)
    value_half = value_acc.astype(jnp.bfloat16)
    source_grad = jnp.dot(key_half, key_weight.T, preferred_element_type=jnp.float32) + jnp.dot(value_half, value_weight.T, preferred_element_type=jnp.float32)
    key_grad = jnp.dot(key_half.T, source, preferred_element_type=jnp.float32) * (1.0 / math.sqrt(source.shape[0]))
    return (query_grad, source_grad, key_grad)
```

```python
import functools
import math

import jax
import jax.numpy as jnp
from jax import lax
from jax.experimental import pallas as pl
from jax.experimental.pallas import tpu as pltpu
from jax.sharding import PartitionSpec as P

KV_HEADS = 2
HEAD_DIM = 128
Y_N = 4
LOG2E = 1.0 / math.log(2.0)
MESH = pl.DeviceIdType.MESH
F32 = jnp.float32
BF16 = jnp.bfloat16


def dot_nt(left, right, precision=None):
    return lax.dot_general(
        left, right, (((1,), (1,)), ((), ())), preferred_element_type=F32, precision=precision
    )


def dot_tn(left, right):
    return lax.dot_general(left, right, (((0,), (0,)), ((), ())), preferred_element_type=F32)


def dot_nn(left, right):
    return jnp.dot(left, right, preferred_element_type=F32)


def kernel(
    y_n, z_n, tp_n, src_total,
    q_ref, o_ref, d_ref, lse_ref, key_ref, value_ref, source_ref,
    dq_ref, kv_ref, kg_ref,
    qd, stats, kvs, acc, dq_acc, dq_out, dq_in, pair_out, pair_in, g_own, g_out, g_in, tp_in,
    src, ky_out, ky_in, z_own, z_out, z_in,
    copy_sem, q_s, q_r, k_s, k_r, kf_s, kf_r, dq_s, dq_r, p_s, p_r, g_s, g_r, t_s, t_r, tf_s, tf_r,
    ky_s, ky_r, z_s, z_r,
):
    sp = lax.axis_index("sp")
    tp = lax.axis_index("tp")
    z, y = sp // y_n, sp % y_n
    x, c = tp // 2, tp % 2
    x_n = tp_n // 2
    per_key = tp_n // KV_HEADS
    key_col = pl.multiple_of(tp // per_key * HEAD_DIM, HEAD_DIM)
    half = z_n // 2
    rows = q_ref.shape[0]
    src_rows = key_ref.shape[0]
    hr = src_rows // 2
    scale = 1.0 / math.sqrt(HEAD_DIM)

    def zd(k):
        return {"sp": lax.rem(z + k + z_n, z_n) * y_n + y, "tp": tp}

    def yd(k):
        return {"sp": z * y_n + lax.rem(y + k + y_n, y_n), "tp": tp}

    def xd(k):
        return {"sp": sp, "tp": lax.rem(x + k + x_n, x_n) * 2 + c}

    partner = {"sp": sp, "tp": x * 2 + 1 - c}

    def remote(source, target, send, recv, device):
        return pltpu.make_async_remote_copy(
            src_ref=source, dst_ref=target, send_sem=send, recv_sem=recv,
            device_id=device, device_id_type=MESH,
        )

    load = pltpu.make_async_copy(source_ref, src, copy_sem)
    load.start()
    barrier = pltpu.get_barrier_semaphore()
    greet = [zd(1), zd(-1)] + [yd(k) for k in range(1, y_n)]
    greet += [xd(k) for k in range(1, x_n)] + [partner]
    for device in greet:
        pl.semaphore_signal(barrier, inc=1, device_id=device, device_id_type=MESH)
    prod = d_ref[...].astype(F32) * o_ref[...].astype(F32)
    delta = dot_nt(jnp.ones((8, HEAD_DIM), F32), prod, lax.Precision.HIGHEST)
    for way in range(2):
        stats[way, 0, 0:1, :] = lse_ref[0:1, :] * LOG2E
        stats[way, 0, 1:2, :] = delta[0:1, :]
    kvs[0, 0] = key_ref[:, pl.ds(key_col, HEAD_DIM)]
    kvs[0, 1] = value_ref[:, pl.ds(key_col, HEAD_DIM)]
    pl.semaphore_wait(barrier, len(greet))

    steps = [zd(1), zd(-1)]

    def q_copy(way, d, i):
        if i == 2:
            source, target = stats.at[way, d], stats.at[way, d + 1]
        else:
            source = (q_ref, d_ref)[i] if d == 0 else qd.at[way, d, i]
            target = qd.at[way, d + 1, i]
        return remote(source, target, q_s.at[way, d, i], q_r.at[way, d + 1, i], steps[way])

    def pieces(way, d):
        if d < half:
            return (2, 0, 1)
        return (2, 0) if way == 0 else (1,)

    def relay(d):
        for i in (2, 0, 1):
            for way in range(2):
                if d > 0 and i in pieces(way, d):
                    q_copy(way, d - 1, i).wait_recv()
                if d < half and i in pieces(way, d + 1):
                    q_copy(way, d, i).start()

    def k_copy(k):
        return remote(
            kvs.at[0, c], kvs.at[y_n - k, c], k_s.at[k], k_r.at[y_n - k], yd(k)
        )

    lo, hi = pl.ds(0, hr), pl.ds(hr, hr)
    k_relays = (
        remote(kvs.at[3, c, lo], kvs.at[2, c, lo], k_s.at[0], k_r.at[0], yd(1)),
        remote(kvs.at[1, c, hi], kvs.at[2, c, hi], k_s.at[2], k_r.at[2], yd(-1)),
    )

    def k_pass(k, role):
        return remote(kvs.at[k, role], kvs.at[k, role], kf_s.at[k], kf_r.at[k], partner)

    def got_sides():
        for k in (3, 1):
            k_copy(y_n - k).wait_recv()
            k_relays[0 if k == 3 else 1].start()
            k_pass(k, c).start()
        for k in (3, 1):
            k_pass(k, 1 - c).wait_recv()

    def got_across():
        for copy in k_relays:
            copy.wait_recv()
        k_pass(2, c).start()
        k_pass(2, 1 - c).wait_recv()

    seen = set()

    def add(ref, key, value):
        if key in seen:
            ref[...] += value
        else:
            ref[...] = value
            seen.add(key)

    def tile(d, blocks):
        if d == 0:
            q, g = q_ref[...], d_ref[...]
            lse, delta = stats[0, 0, 0:1, :], stats[0, 0, 1:2, :]
        elif d == half:
            q, g = qd[0, d, 0], qd[1, d, 1]
            lse, delta = stats[0, d, 0:1, :], stats[0, d, 1:2, :]
        else:
            q = jnp.concatenate([qd[0, d, 0], qd[1, d, 0]], axis=0)
            g = jnp.concatenate([qd[0, d, 1], qd[1, d, 1]], axis=0)
            lse = jnp.concatenate([stats[0, d, 0:1, :], stats[1, d, 0:1, :]], axis=1)
            delta = jnp.concatenate([stats[0, d, 1:2, :], stats[1, d, 1:2, :]], axis=1)
        for s in blocks:
            k, v = kvs[s, 0], kvs[s, 1]
            probs = jnp.exp2(dot_nt(k, q) * (scale * LOG2E) - lse)
            dscores = (probs * (dot_nt(v, g) - delta)).astype(BF16)
            add(acc.at[1, s], ("v", s), dot_nn(probs.astype(BF16), g))
            add(acc.at[0, s], ("k", s), dot_nn(dscores, q))
            add(dq_acc.at[d, pl.ds(0, q.shape[0])], ("q", d), dot_tn(dscores, k))

    def dq_copy(way, d):
        return remote(
            dq_out.at[d, pl.ds(way * rows, rows)], dq_in.at[d, pl.ds(way * rows, rows)],
            dq_s.at[d, way], dq_r.at[d, way], zd(d if way else -d),
        )

    def ways(d):
        return range(1 if d == half else 2)

    def send_dq(d):
        span = pl.ds(0, rows * len(ways(d)))
        dq_out[d, span] = (dq_acc[d, span] * scale).astype(BF16)
        for way in ways(d):
            dq_copy(way, d).start()

    mine, other = pl.ds(pl.multiple_of(c * hr, hr), hr), pl.ds(pl.multiple_of((1 - c) * hr, hr), hr)

    def pair_copy(i, k):
        return remote(pair_out.at[i, k], pair_in.at[i, k], p_s.at[i, k], p_r.at[i, k], partner)

    def send_pair(k):
        for i in range(2):
            part = acc[i, k, other, :]
            pair_out[i, k] = (part if i else part * scale).astype(BF16)
            pair_copy(i, k).start()

    def g_copy(i, k):
        return remote(
            g_out.at[i, k], g_in.at[i, y_n - k], g_s.at[i, k], g_r.at[i, y_n - k], yd(k)
        )

    order = (2, 1, 3, 0)
    relay(0)
    for k in (1, 3):
        k_copy(k).start()
    tile(0, (0,))
    relay(1)
    if half > 1:
        tile(1, (0,))
    got_sides()
    late = {0: (0,), 1: (0,)}
    for d in range(2, half):
        relay(d)
        if d == 2:
            tile(0, (1, 3))
            tile(1, (1, 3))
            tile(2, (0, 1, 3))
            got_across()
        elif d == 3:
            tile(3, (0, 1, 2, 3))
            tile(0, (2,))
            tile(1, (2,))
            tile(2, (2,))
        else:
            tile(d, (0, 1, 2, 3))
    if half == 2:
        tile(0, (1, 3))
        tile(1, (1, 3))
        got_across()
        tile(0, (2,))
        tile(1, (2,))
    elif half == 3:
        tile(0, (2,))
        tile(1, (2,))
        tile(2, (2,))
    relay(half)
    for d in range(1, half):
        send_dq(d)
    for k in order:
        tile(half, (k,))
        send_pair(k)
    send_dq(half)

    def reduce_pair(i):
        for k in order:
            pair_copy(i, k).wait_recv()
            part = acc[i, k, mine, :]
            total = (part if i else part * scale) + pair_in[i, k].astype(F32)
            if k:
                g_out[i, k] = total.astype(BF16)
                g_copy(i, k).start()
            else:
                g_own[i] = total

    def tp_copy(i, k):
        return remote(tp_in.at[i, x, c], tp_in.at[i, x, c], t_s.at[i, k], t_r.at[i, x], xd(k))

    def tp_got(i, k):
        other_x = lax.rem(x + k, x_n)
        return remote(
            tp_in.at[i, other_x, c], tp_in.at[i, other_x, c], t_s.at[i, k], t_r.at[i, other_x], xd(k)
        )

    def tp_pass(i, k, role):
        at = lax.rem(x + k, x_n)
        return remote(
            tp_in.at[i, at, role], tp_in.at[i, at, role], tf_s.at[i, at], tf_r.at[i, at], partner
        )

    def reduce_sites(i):
        total = g_own[i]
        for k in range(1, y_n):
            g_copy(i, y_n - k).wait_recv()
            total += g_in[i, k].astype(F32)
        tp_in[i, x, c] = total.astype(BF16)
        for k in range(1, x_n):
            tp_copy(i, k).start()
        tp_pass(i, 0, c).start()

    def gather_heads(i):
        for k in range(1, x_n):
            tp_got(i, k).wait_recv()
            tp_pass(i, k, c).start()
        for k in range(x_n):
            tp_pass(i, k, 1 - c).wait_recv()
        chips = x_n // KV_HEADS
        for g in range(KV_HEADS):
            for r in range(2):
                total = tp_in[i, g * chips, r]
                if chips > 1:
                    total = total.astype(F32)
                    for p in range(1, chips):
                        total += tp_in[i, g * chips + p, r].astype(F32)
                col = (i * KV_HEADS + g) * HEAD_DIM
                kv_ref[r * hr : (r + 1) * hr, col : col + HEAD_DIM] = total.astype(BF16)

    reduce_pair(0)
    reduce_pair(1)
    reduce_sites(0)
    load.wait()
    reduce_sites(1)
    gather_heads(0)

    width = KV_HEADS * HEAD_DIM
    part = width // (y_n * z_n)
    to = lax.broadcasted_iota(jnp.int32, (width, width), 1)
    at = lax.broadcasted_iota(jnp.int32, (width, width), 0)
    home = (to % (z_n * part)) // part * (y_n * part) + to // (z_n * part) * part + to % part
    pick = jnp.where(at == home, 1.0, 0.0).astype(BF16)
    key_half = dot_nn(kv_ref[:, 0:width], pick).astype(BF16)
    partial = dot_tn(key_half, src[...]) * (1.0 / math.sqrt(src_total))
    for k in range(y_n):
        ky_out[k] = partial[k * z_n * part : (k + 1) * z_n * part].astype(BF16)

    def ky_copy(k):
        return remote(
            ky_out.at[lax.rem(y + k, y_n)], ky_in.at[y_n - k], ky_s.at[k], ky_r.at[y_n - k], yd(k)
        )

    for k in (2, 1, 3):
        ky_copy(k).start()

    gather_heads(1)

    total = ky_out[y].astype(F32)
    for k in range(1, y_n):
        ky_copy(y_n - k).wait_recv()
        total += ky_in[k].astype(F32)
    for k in range(z_n):
        z_own[k] = total[k * part : (k + 1) * part]
        z_out[k] = total[k * part : (k + 1) * part].astype(BF16)

    def z_copy(k):
        return remote(
            z_out.at[lax.rem(z + k, z_n)], z_in.at[z_n - k], z_s.at[k], z_r.at[z_n - k], zd(k)
        )

    far = sorted(range(1, z_n), key=lambda k: -min(k, z_n - k))
    for k in far:
        z_copy(k).start()

    total = dq_acc[0, pl.ds(0, rows)] * scale
    for d in range(1, half + 1):
        for way in ways(d):
            dq_copy(way, d).wait_recv()
            total += dq_in[d, pl.ds(way * rows, rows)].astype(F32)
    dq_ref[...] = total

    total = z_own[z]
    for k in reversed(far):
        z_copy(z_n - k).wait_recv()
        total += z_in[k].astype(F32)
    kg_ref[...] = total

    for d in range(half):
        for way in range(2):
            for i in pieces(way, d + 1):
                q_copy(way, d, i).wait_send()
    for d in range(1, half + 1):
        for way in ways(d):
            dq_copy(way, d).wait_send()
    for k in (1, 3):
        k_copy(k).wait_send()
    for copy in k_relays:
        copy.wait_send()
    for k in range(1, y_n):
        k_pass(k, c).wait_send()
        ky_copy(k).wait_send()
    for i in range(2):
        for k in range(y_n):
            pair_copy(i, k).wait_send()
            if k:
                g_copy(i, k).wait_send()
        for k in range(x_n):
            tp_pass(i, k, c).wait_send()
            if k:
                tp_copy(i, k).wait_send()
    for k in far:
        z_copy(k).wait_send()


def finish_kernel(
    kv_hbm, kw_hbm, vw_hbm, dq_hbm, kg_hbm, out_ref, dq_out, kg_out,
    kv, kw, vw, dq, kg, buf, in_sems, w_sems, out_sems, pass_sems,
):
    half = kw.shape[1]
    width = buf.shape[2]
    count = buf.shape[0]
    load = pltpu.make_async_copy(kv_hbm, kv, in_sems.at[0])
    load.start()
    loads = []
    for n in range(count):
        cols = pl.ds(n * width, width)
        loads.append(
            [
                pltpu.make_async_copy(ref.at[cols], to.at[cols], w_sems.at[n, i])
                for i, (ref, to) in enumerate(((kw_hbm, kw), (vw_hbm, vw)))
            ]
        )
        for copy in loads[n]:
            copy.start()
    dq_in = pltpu.make_async_copy(dq_hbm, dq, in_sems.at[1])
    kg_in = pltpu.make_async_copy(kg_hbm, kg, in_sems.at[2])
    dq_in.start()
    kg_in.start()
    load.wait()
    copies = []
    for n in range(count):
        cols = slice(n * width, (n + 1) * width)
        for copy in loads[n]:
            copy.wait()
        buf[n] = dot_nt(kv[:, :half], kw[cols]) + dot_nt(kv[:, half:], vw[cols])
        copies.append(
            pltpu.make_async_copy(
                buf.at[n], out_ref.at[:, pl.ds(n * width, width)], out_sems.at[n]
            )
        )
        copies[n].start()
    dq_in.wait()
    copies.append(pltpu.make_async_copy(dq, dq_out, pass_sems.at[0]))
    copies[-1].start()
    kg_in.wait()
    copies.append(pltpu.make_async_copy(kg, kg_out, pass_sems.at[1]))
    copies[-1].start()
    for copy in copies:
        copy.wait()

def shards(
    y_n, z_n, tp_n,
    queries, attn_out, out_grad, row_lse, source, saved_keys, saved_values, key_weight, value_weight
):
    rows, width = queries.shape
    src_rows, columns = source.shape
    kv_width = KV_HEADS * HEAD_DIM
    sp_n = y_n * z_n
    part = kv_width // sp_n
    half = z_n // 2
    x_n = tp_n // 2
    hr = src_rows // 2
    dma = pltpu.SemaphoreType.DMA
    vmem = pl.BlockSpec(memory_space=pltpu.VMEM)
    scratch = [
        pltpu.VMEM((2, half + 1, 2, rows, width), BF16),
        pltpu.VMEM((2, half + 1, 2, rows), F32),
        pltpu.VMEM((y_n, 2, src_rows, HEAD_DIM), BF16),
        pltpu.VMEM((2, y_n, src_rows, HEAD_DIM), F32),
        pltpu.VMEM((half + 1, 2 * rows, HEAD_DIM), F32),
        pltpu.VMEM((half + 1, 2 * rows, HEAD_DIM), BF16),
        pltpu.VMEM((half + 1, 2 * rows, HEAD_DIM), BF16),
        pltpu.VMEM((2, y_n, hr, HEAD_DIM), BF16),
        pltpu.VMEM((2, y_n, hr, HEAD_DIM), BF16),
        pltpu.VMEM((2, hr, HEAD_DIM), F32),
        pltpu.VMEM((2, y_n, hr, HEAD_DIM), BF16),
        pltpu.VMEM((2, y_n, hr, HEAD_DIM), BF16),
        pltpu.VMEM((2, x_n, 2, hr, HEAD_DIM), BF16),
        pltpu.VMEM((src_rows, columns), BF16),
        pltpu.VMEM((y_n, z_n * part, columns), BF16),
        pltpu.VMEM((y_n, z_n * part, columns), BF16),
        pltpu.VMEM((z_n, part, columns), F32),
        pltpu.VMEM((z_n, part, columns), BF16),
        pltpu.VMEM((z_n, part, columns), BF16),
        dma,
    ]
    for shape in (
        (2, half + 1, 3), (2, half + 1, 3), (y_n,), (y_n,), (y_n,), (y_n,), (half + 1, 2), (half + 1, 2),
        (2, y_n), (2, y_n), (2, y_n), (2, y_n), (2, x_n), (2, x_n), (2, x_n), (2, x_n),
        (y_n,), (y_n,), (z_n,), (z_n,),
    ):
        scratch.append(dma(shape))
    query_grad, kv_half, key_grad = pl.pallas_call(
        functools.partial(kernel, y_n, z_n, tp_n, src_rows * sp_n),
        out_shape=(
            jax.ShapeDtypeStruct((rows, width), F32),
            jax.ShapeDtypeStruct((src_rows, 2 * kv_width), BF16),
            jax.ShapeDtypeStruct((part, columns), F32),
        ),
        in_specs=[vmem] * 6 + [pl.BlockSpec(memory_space=pl.ANY)],
        out_specs=(vmem, vmem, vmem),
        scratch_shapes=scratch,
        compiler_params=pltpu.CompilerParams(
            collective_id=0, has_side_effects=True, vmem_limit_bytes=60 * 2**20
        ),
        name="attention_grads",
    )(queries, attn_out, out_grad, row_lse.T, saved_keys, saved_values, source)
    local_columns = key_weight.shape[0]
    blocks = local_columns // math.gcd(local_columns, 256)
    hbm = pl.BlockSpec(memory_space=pl.ANY)
    source_grad, query_grad, key_grad = pl.pallas_call(
        finish_kernel,
        out_shape=(
            jax.ShapeDtypeStruct((src_rows, local_columns), F32),
            jax.ShapeDtypeStruct((rows, width), F32),
            jax.ShapeDtypeStruct((part, columns), F32),
        ),
        in_specs=[hbm] * 5,
        out_specs=(hbm, hbm, hbm),
        scratch_shapes=[
            pltpu.VMEM((src_rows, 2 * kv_width), BF16),
            pltpu.VMEM((local_columns, kv_width), BF16),
            pltpu.VMEM((local_columns, kv_width), BF16),
            pltpu.VMEM((rows, width), F32),
            pltpu.VMEM((part, columns), F32),
            pltpu.VMEM((blocks, src_rows, local_columns // blocks), F32),
            dma((3,)),
            dma((blocks, 2)),
            dma((blocks,)),
            dma((2,)),
        ],
        compiler_params=pltpu.CompilerParams(vmem_limit_bytes=60 * 2**20),
        name="source_grads",
    )(kv_half, key_weight, value_weight, query_grad, key_grad)
    return (query_grad, source_grad, key_grad)


def solution(mesh):
    sp_n, tp_n = mesh.shape["sp"], mesh.shape["tp"]
    in_specs = (
        P("sp", "tp"),
        P("sp", "tp"),
        P("sp", "tp"),
        P("sp", "tp"),
        P("sp", "tp"),
        P("sp", None),
        P("sp", None),
        P("tp", None),
        P("tp", None),
    )
    out_specs = (P("sp", "tp"), P("sp", "tp"), P("sp", "tp"))
    return jax.shard_map(
        functools.partial(shards, Y_N, sp_n // Y_N, tp_n),
        mesh=mesh, in_specs=in_specs, out_specs=out_specs, check_vma=False,
    )
```
